32 devices in a mesh: ep: 4 (over z), tp: 8 (over y, x, core).
Axes of the slice: x: 2, y: 2, z: 4, core: 2. Of those that a mesh axis runs over, the one named last changes fastest.
Arguments:
- tokens: bfloat16 [512, 2048], P('ep'), may hold values from -6 to 6
- norm_gain: float32 [2048], replicated, may hold values from 0.1 to 1.9
- route_ids: int32 [512, 2], P('ep'), may hold values from 0 to 3, all different within a row; in each aligned block of 128 rows (0 to 127, 128 to 255, ...) at most 96 rows name the same one
- route_weights: float32 [512, 2], P('ep'), may hold values from 0.05 to 1
- gate_proj: bfloat16 [4, 2048, 12288], P('ep', None, 'tp'), may hold values from -0.125 to 0.125
- up_proj: bfloat16 [4, 2048, 12288], P('ep', None, 'tp'), may hold values from -0.125 to 0.125
- down_proj: bfloat16 [4, 12288, 2048], P('ep', 'tp'), may hold values from -0.0546875 to 0.0546875
Outputs:
- mixed: bfloat16 [512, 2048], P('ep', 'tp')
The draws below stay inside these ranges and needn't reach their ends.
Inputs may be any that keep to these rules, and one draw needn't show every extreme that they name: `route_ids`: each token names 2 different experts; within the rows of one device (aligned blocks of 128 tokens) no expert is named by more than 96 pairs, a bound that some block reaches.
All inputs are finite; a program needn't handle non-finite values.
Results may differ from the reference program's by a relative error of at most 0.017.
Values may be sent and summed in bfloat16 or wider, within the bound.
A program may use at most 64 MiB of HBM per device.

```python
import math
import jax
import jax.numpy as jnp
import numpy as np
from jax import lax

D = 2048
FF = 12288
TOPK = 2
TOK_DEV = 128
EXPERTS = 4
TOKENS = 512
CAP = 96
HID_BLOCK = 1536
N_EP = 4
N_TP = 8


def levels(key, shape, cuts, smallest, largest):
    level, own = 1.0, jax.random.fold_in(key, 6)
    for axis_at, shards_of in cuts:
        draws = jnp.exp(jax.random.uniform(jax.random.fold_in(own, axis_at), (shards_of,), jnp.float32, smallest / len(cuts), largest / len(cuts)))
        level = level * jnp.repeat(draws, shape[axis_at] // shards_of).reshape([-1 if axis == axis_at else 1 for axis in range(len(shape))])
    return level


def assign_block(rng, own, number, rows, count, top, most, skew):
    ranking = jax.random.permutation(rng, count)
    packed, common = shares(count, rows * top, most, skew, True), shares(count, rows * top, most, skew, False)
    places = jnp.arange(count)

    def named(tallies, offset_by):
        used = int((tallies > 0).sum())
        fixed = max(1, used // 4)
        shifted = fixed + (places - fixed + offset_by * (used - fixed)) % max(1, count - fixed)
        return jnp.zeros((count,), jnp.int32).at[ranking[jnp.where(places < fixed, places, shifted)]].set(jnp.asarray(tallies, jnp.int32))

    tallies = jnp.where(number % 4 == 0, named(packed, number // 4), named(common, number - number // 4 - 1))
    mixed = jax.random.permutation(jax.random.fold_in(own, 3), count)
    giver, receiver = mixed[0:count // 2 * 2:2], mixed[1:count // 2 * 2:2]
    slack = jnp.minimum(tallies[giver] - 1, most - tallies[receiver]) // 2
    slack = jnp.where((giver == ranking[0]) | (receiver == ranking[0]) | (tallies[receiver] == 0), 0, jnp.maximum(slack, 0))
    shifted = jax.random.randint(jax.random.fold_in(own, 4), (count // 2,), 0, 1 << 20) % (slack + 1)
    tallies = tallies.at[giver].add(-shifted).at[receiver].add(shifted)
    members = jnp.searchsorted(jnp.cumsum(tallies), jnp.arange(rows * top), side="right").astype(jnp.int32)
    listing = members.reshape(top, rows).T
    listing = listing[jax.random.permutation(jax.random.fold_in(own, 1), rows)]
    offset_by = jax.random.randint(jax.random.fold_in(own, 2), (rows, 1), 0, top)
    return jnp.take_along_axis(listing, (jnp.arange(top)[None, :] + offset_by) % top, axis=1)


def shares(amount, total, limit, slope, full):
    portions = [(1 << 20) // math.isqrt(standing ** slope) + 1 for standing in range(1, amount + 1)]
    largest = limit if full else min(limit, max(-(-total // amount), total * portions[0] // sum(portions)))
    least = 1 if total - largest >= amount - 1 else 0
    holding, rest = [largest] + [least] * (amount - 1), total - largest - least * (amount - 1)
    while rest > 0:
        candidates = [i for i in range(1, amount) if holding[i] < largest] or [i for i in range(1, amount) if holding[i] < limit]
        whole, remaining = sum([portions[i] for i in candidates]), rest
        for i in candidates:
            addition = min(limit - holding[i], max(1, remaining * portions[i] // whole), rest)
            holding[i] = holding[i] + addition
            rest = rest - addition
    return np.array(holding)


def normal_values(key, extent, deviation, most, pieces=(), kind=jnp.bfloat16):
    level = levels(key, extent, pieces, -0.22, 0.18) if pieces else 1.0
    array = jax.random.normal(key, extent, jnp.float32) * deviation * level
    return jnp.minimum(jnp.maximum(array, -most), most).astype(kind)


def setup_inputs(seed: int = 0) -> dict:
    seeds = jax.random.split(jax.random.key(seed), 8)
    tokens = normal_values(seeds[0], (TOKENS, D), 1.0, 6.0, ((0, 4),))
    norm_gain = jnp.clip(1.0 + 0.18 * jax.random.normal(seeds[1], (D,), jnp.float32), 0.1, 1.9)
    route_ids_keys = jax.random.split(jax.random.fold_in(seeds[2], 1), TOKENS // TOK_DEV)
    route_ids_turns = jax.random.permutation(jax.random.fold_in(seeds[2], 3), TOKENS // TOK_DEV)
    route_ids = jax.vmap(lambda own, number: assign_block(jax.random.fold_in(seeds[2], 2), own, number, TOK_DEV, EXPERTS, TOPK, CAP, 2))(route_ids_keys, route_ids_turns).reshape((TOKENS, TOPK))
    route_weights = jnp.clip(jnp.exp(math.log(1.0) - 2.9957323 * jax.random.uniform(seeds[3], (TOKENS, TOPK), jnp.float32) ** levels(seeds[3], (TOKENS, TOPK), ((0, 4),), -0.2, 0.2)), 0.05, 1.0)
    gate_proj = normal_values(seeds[4], (EXPERTS, D, FF), D ** -0.5, 0.125, ((0, 4), (2, 8)))
    up_proj = normal_values(seeds[5], (EXPERTS, D, FF), D ** -0.5, 0.125, ((0, 4), (2, 8)))
    down_proj = normal_values(seeds[6], (EXPERTS, FF, D), FF ** -0.5, 0.0546875, ((0, 4), (1, 8)))
    return dict(tokens=tokens, norm_gain=norm_gain, route_ids=route_ids, route_weights=route_weights, gate_proj=gate_proj, up_proj=up_proj, down_proj=down_proj)


def reference(tokens, norm_gain, route_ids, route_weights, gate_proj, up_proj, down_proj):
    values = tokens.astype(jnp.float32)
    mean_square = lax.optimization_barrier(jnp.mean(values * values, axis=-1, keepdims=True))
    normed = (values * lax.rsqrt(mean_square + 1e-06) * norm_gain).astype(jnp.bfloat16)
    route_flat = route_ids.reshape(N_EP, TOK_DEV * TOPK)
    onehot = (route_flat[:, :, None] == jnp.arange(EXPERTS, dtype=jnp.int32)[None, None, :]).astype(jnp.int32)
    earlier = jnp.cumsum(onehot, axis=1) - onehot
    slot_index = lax.optimization_barrier(jnp.sum(earlier * onehot, axis=-1)).astype(jnp.int32)
    source_ids = jnp.arange(N_EP, dtype=jnp.int32)[:, None]
    buffer_row = (source_ids * CAP + slot_index).reshape(-1)
    expert_ids = route_flat.reshape(-1)
    repeated = jnp.repeat(normed, TOPK, axis=0)
    buffers = jnp.zeros((EXPERTS, N_EP * CAP, D), jnp.bfloat16).at[expert_ids, buffer_row].set(repeated)

    def expert(operands):
        rows_in, gate_w, up_w, down_w = operands
        gate_act = jnp.dot(rows_in, gate_w, preferred_element_type=jnp.float32)
        up_act = jnp.dot(rows_in, up_w, preferred_element_type=jnp.float32)
        hidden = (jax.nn.silu(gate_act) * up_act).astype(jnp.bfloat16)
        hidden_blocks = hidden.reshape(N_EP * CAP, N_TP, HID_BLOCK).astype(jnp.float32)
        down_blocks = down_w.reshape(N_TP, HID_BLOCK, D).astype(jnp.float32)
        partial_value = jnp.einsum('rbf,bfd->brd', hidden_blocks, down_blocks).astype(jnp.bfloat16)
        partial_value = lax.optimization_barrier(partial_value)
        return lax.optimization_barrier(jnp.sum(partial_value.astype(jnp.float32), axis=0))
    results = lax.map(expert, (buffers, gate_proj, up_proj, down_proj))
    picked = results[expert_ids, buffer_row].reshape(TOKENS, TOPK, D)
    mixed = lax.optimization_barrier(jnp.sum(route_weights[:, :, None] * picked, axis=1))
    return mixed.astype(jnp.bfloat16)
```

```python
import functools

import jax
import jax.numpy as jnp
from jax import lax
from jax.experimental import pallas as pl
from jax.experimental.pallas import tpu as pltpu
from jax.sharding import PartitionSpec as P

MESH = pl.DeviceIdType.MESH
F32, BF16 = jnp.float32, jnp.bfloat16


def dot(a, b):
    return jnp.dot(a, b, preferred_element_type=F32)


def fused(ep, cap, share, chunk, tok, gain, ids, wts, gate_h, up_h, down_h, out, *scratch):
    (normed, pick, rows, outbox, gate_w, up_w, down_w, hidden, to_sib, from_sib, acc, sent, from_diag,
     from_x, from_y, relay, final, back, wsem, ssem, rsem) = scratch
    toks, width = tok.shape
    topk = ids.shape[0]
    hid = hidden.shape[1]
    total = ep * cap
    half = total // 2
    e = lax.axis_index("ep")
    j = lax.axis_index("tp")
    c, x, y = j % 2, (j // 2) % 2, j // 4

    def at(yy, xx, cc):
        return (yy * 2 + xx) * 2 + cc

    spots = [(y, x), (y, 1 - x), (1 - y, x), (1 - y, 1 - x)]

    def cols(m, core):
        return pl.ds(pl.multiple_of(at(*spots[m], core) * share, share), share)

    x_dev = (e, at(y, 1 - x, c))
    y_dev = (e, at(1 - y, x, c))
    sib = (e, at(y, x, 1 - c))
    dists = list(range(1, ep))
    near = sorted(dists, key=lambda d: min(d, ep - d))

    loads = [
        pltpu.make_async_copy(h.at[0], v, wsem.at[i])
        for i, (h, v) in enumerate(((gate_h, gate_w), (up_h, up_w), (down_h, down_w)))
    ]
    for load in loads:
        load.start()
    barrier = pltpu.get_barrier_semaphore()
    greeted = [((e + d) % ep, j) for d in dists] + [x_dev, y_dev, sib]
    for dev in greeted:
        pl.semaphore_signal(barrier, inc=1, device_id=dev, device_id_type=MESH)

    count = [0]
    started = []

    def remote(src, dst, dev):
        k = count[0]
        count[0] += 1
        copy = pltpu.make_async_remote_copy(
            src_ref=src, dst_ref=dst, send_sem=ssem.at[k], recv_sem=rsem.at[k],
            device_id=dev, device_id_type=MESH,
        )
        started.append(copy)
        copy.start()
        return copy

    values = tok[...].astype(F32)
    mean_square = jnp.mean(values * values, axis=-1, keepdims=True)
    normed[...] = (values * lax.rsqrt(mean_square + 1e-06) * gain[...]).astype(BF16)
    experts = lax.broadcasted_iota(jnp.int32, (8 * ((ep + 7) // 8), toks), 0)
    named = jnp.zeros(experts.shape, jnp.bool_)
    for k in range(topk):
        named = named | (ids[k : k + 1, :] == experts)
    named = jnp.where(named, 1.0, 0.0)
    before = (
        lax.broadcasted_iota(jnp.int32, (toks, toks), 0)
        < lax.broadcasted_iota(jnp.int32, (toks, toks), 1)
    )
    slot = dot(named.astype(BF16), jnp.where(before, 1.0, 0.0).astype(BF16))
    place = jnp.where(named > 0.5, slot, -1.0)
    slots = lax.broadcasted_iota(jnp.int32, (cap, toks), 0).astype(F32)
    for s in range(ep):
        pick[s] = jnp.where(place[s : s + 1, :] == slots, 1.0, 0.0).astype(BF16)
    mine = cols(0, c)
    for d in dists:
        outbox[d - 1] = dot(pick[(e + d) % ep], normed[:, mine]).astype(BF16)

    pl.semaphore_wait(barrier, len(greeted))
    over_z = {}
    for d in sorted(dists, key=lambda d: -min(d, ep - d)):
        over_z[d] = remote(outbox.at[d - 1], rows.at[e, :, mine], ((e + d) % ep, j))
    rows[e] = dot(pick[e], normed[...]).astype(BF16)

    along_x, along_y, diag_1, diag_2, over_d2d = {}, {}, {}, {}, []
    quarter = share // 2

    def piece(s, m, part=None):
        if part is None:
            return rows.at[s, :, cols(m, c)]
        start = pl.multiple_of(at(*spots[m], c) * share + part * quarter, quarter)
        return rows.at[s, :, pl.ds(start, quarter)]

    for t in range(len(near) + 2):
        if t < len(near):
            d = near[t]
            s = (e + ep - d) % ep
            over_z[d].wait_recv()
            along_x[d] = remote(piece(s, 0), piece(s, 0), x_dev)
            along_y[d] = remote(piece(s, 0), piece(s, 0), y_dev)
            over_d2d.append(remote(piece(s, 0), piece(s, 0), sib))
        if 0 <= t - 1 < len(near):
            d = near[t - 1]
            s = (e + ep - d) % ep
            along_x[d].wait_recv()
            diag_1[d] = remote(piece(s, 1, 0), piece(s, 1, 0), y_dev)
            over_d2d.append(remote(piece(s, 1), piece(s, 1), sib))
            along_y[d].wait_recv()
            diag_2[d] = remote(piece(s, 2, 1), piece(s, 2, 1), x_dev)
            over_d2d.append(remote(piece(s, 2), piece(s, 2), sib))
        if 0 <= t - 2:
            d = near[t - 2]
            s = (e + ep - d) % ep
            diag_1[d].wait_recv()
            diag_2[d].wait_recv()
            over_d2d.append(remote(piece(s, 3), piece(s, 3), sib))
    loads[0].wait()
    loads[1].wait()
    for copy in over_d2d:
        copy.wait_recv()

    @pl.loop(0, hid // chunk)
    def _(n):
        at_n = pl.ds(pl.multiple_of(n * chunk, chunk), chunk)
        held = rows[...].reshape(total, width)
        gate_act = dot(held, gate_w[:, at_n])
        up_act = dot(held, up_w[:, at_n])
        hidden[:, at_n] = (gate_act / (1.0 + jnp.exp(-gate_act)) * up_act).astype(BF16)

    loads[2].wait()
    pair = {}

    def compute(m):
        to_sib[m] = dot(hidden[...], down_w[:, cols(m, 1 - c)]).astype(BF16)
        pair[m] = remote(to_sib.at[m], from_sib.at[m], sib)
        acc[m] = dot(hidden[...], down_w[:, cols(m, c)])

    def joined(m):
        pair[m].wait_recv()
        return acc[m] + from_sib[m].astype(F32)

    low, high = pl.ds(0, half), pl.ds(half, half)
    compute(3)
    compute(1)
    sent[0] = joined(3).astype(BF16)
    diag_a = remote(sent.at[0, low], from_diag.at[0], x_dev)
    diag_b = remote(sent.at[0, high], from_diag.at[1], y_dev)
    compute(2)
    along = joined(1)
    sent[1, :half] = along[:half].astype(BF16)
    acc[1] = along
    x_a = remote(sent.at[1, low], from_x.at[0], x_dev)
    compute(0)
    along = joined(2)
    sent[2, half:] = along[half:].astype(BF16)
    acc[2] = along
    y_b = remote(sent.at[2, high], from_y.at[1], y_dev)
    diag_a.wait_recv()
    relay[0] = (acc[2, :half] + from_diag[0].astype(F32)).astype(BF16)
    y_a = remote(relay.at[0], from_y.at[0], y_dev)
    diag_b.wait_recv()
    relay[1] = (acc[1, half:] + from_diag[1].astype(F32)).astype(BF16)
    x_b = remote(relay.at[1], from_x.at[1], x_dev)
    acc[0] = joined(0)
    for i, (one, two) in enumerate(((x_a, y_a), (y_b, x_b))):
        one.wait_recv()
        two.wait_recv()
        part = acc[0, i * half : (i + 1) * half] + from_x[i].astype(F32) + from_y[i].astype(F32)
        final[i * ep // 2 : (i + 1) * ep // 2] = part.astype(BF16).reshape(ep // 2, cap, share)

    homeward = {}
    for d in sorted(dists, key=lambda d: -min(d, ep - d)):
        s = (e + d) % ep
        homeward[d] = remote(final.at[s], back.at[e], (s, j))
    eye = (
        lax.broadcasted_iota(jnp.int32, (toks, toks), 0)
        == lax.broadcasted_iota(jnp.int32, (toks, toks), 1)
    )

    def weighted(expert, value):
        scale = jnp.zeros((1, toks), F32)
        for k in range(topk):
            scale = scale + jnp.where(ids[k : k + 1, :] == expert, wts[k : k + 1, :], 0.0)
        scale = jnp.sum(jnp.where(eye, scale, 0.0), axis=1, keepdims=True)
        got = lax.dot_general(
            pick[expert], value, (((0,), (0,)), ((), ())), preferred_element_type=F32
        )
        return scale * got

    mixed = weighted(e, final[e])
    for d in near:
        expert = (e + ep - d) % ep
        homeward[d].wait_recv()
        mixed = mixed + weighted(expert, back[expert])
    out[...] = mixed.astype(out.dtype)
    for copy in started:
        copy.wait_send()


def local_fused(tokens, norm_gain, route_ids, route_weights, gate_proj, up_proj, down_proj):
    ep = lax.axis_size("ep")
    tp = lax.axis_size("tp")
    toks, width = tokens.shape
    topk = route_ids.shape[1]
    hid = gate_proj.shape[2]
    cap = capacity_of(toks, topk, ep)
    share = width // tp
    total = ep * cap
    chunk = next(n for n in (256, 128) if hid % n == 0)
    others = ep - 1
    copies = 10 * others + 4 + 6 + others
    vmem = pl.BlockSpec(memory_space=pltpu.VMEM)
    hbm = pl.BlockSpec(memory_space=pltpu.HBM)
    flops = 6 * total * width * hid
    return pl.pallas_call(
        functools.partial(fused, ep, cap, share, chunk),
        out_shape=jax.ShapeDtypeStruct((toks, share), BF16),
        in_specs=[vmem] * 4 + [hbm] * 3,
        out_specs=vmem,
        scratch_shapes=[
            pltpu.VMEM((toks, width), BF16),
            pltpu.VMEM((ep, cap, toks), BF16),
            pltpu.VMEM((ep, cap, width), BF16),
            pltpu.VMEM((others, cap, share), BF16),
            pltpu.VMEM((width, hid), BF16),
            pltpu.VMEM((width, hid), BF16),
            pltpu.VMEM((hid, width), BF16),
            pltpu.VMEM((total, hid), BF16),
            pltpu.VMEM((4, total, share), BF16),
            pltpu.VMEM((4, total, share), BF16),
            pltpu.VMEM((4, total, share), F32),
            pltpu.VMEM((3, total, share), BF16),
            pltpu.VMEM((2, total // 2, share), BF16),
            pltpu.VMEM((2, total // 2, share), BF16),
            pltpu.VMEM((2, total // 2, share), BF16),
            pltpu.VMEM((2, total // 2, share), BF16),
            pltpu.VMEM((ep, cap, share), BF16),
            pltpu.VMEM((ep, cap, share), BF16),
            pltpu.SemaphoreType.DMA((3,)),
            pltpu.SemaphoreType.DMA((copies,)),
            pltpu.SemaphoreType.DMA((copies,)),
        ],
        compiler_params=pltpu.CompilerParams(
            collective_id=0, has_side_effects=True, vmem_limit_bytes=56 * 1024 * 1024
        ),
        cost_estimate=pl.CostEstimate(
            flops=flops, bytes_accessed=6 * width * hid, transcendentals=total * hid
        ),
    )(
        tokens, norm_gain.reshape(1, width), route_ids.T, route_weights.T,
        gate_proj, up_proj, down_proj,
    )


def capacity_of(tok_rows, topk, ep_count):
    return min(tok_rows, (3 * tok_rows * topk + 2 * ep_count - 1) // (2 * ep_count))


def local(tokens, norm_gain, route_ids, route_weights, gate_proj, up_proj, down_proj):
    ep_count = lax.axis_size("ep")
    tp_count = lax.axis_size("tp")
    tok_rows, width = tokens.shape
    topk = route_ids.shape[1]
    capacity = min(tok_rows, (3 * tok_rows * topk + 2 * ep_count - 1) // (2 * ep_count))
    share_width = width // tp_count
    values = tokens.astype(jnp.float32)
    mean_square = jnp.mean(values * values, axis=-1, keepdims=True)
    normed = (values * lax.rsqrt(mean_square + 1e-06) * norm_gain).astype(jnp.bfloat16)
    route_flat = route_ids.reshape(-1)
    onehot = (route_flat[:, None] == jnp.arange(ep_count, dtype=jnp.int32)[None, :]).astype(
        jnp.int32
    )
    slot_index = jnp.sum((jnp.cumsum(onehot, axis=0) - onehot) * onehot, axis=1)
    repeated = jnp.repeat(normed, topk, axis=0)
    down_local = down_proj[0]
    outgoing = (
        jnp.zeros((ep_count, capacity, width), jnp.bfloat16)
        .at[route_flat, slot_index]
        .set(repeated)
    )
    arrived = lax.all_to_all(outgoing, "ep", split_axis=0, concat_axis=0, tiled=True)
    item_rows = arrived.shape[1]
    merged_rows = arrived.reshape(-1, width)
    gate_act = jnp.dot(merged_rows, gate_proj[0], preferred_element_type=jnp.float32)
    up_act = jnp.dot(merged_rows, up_proj[0], preferred_element_type=jnp.float32)
    hidden = (jax.nn.silu(gate_act) * up_act).astype(jnp.bfloat16)
    term = lax.dot_general(
        down_local, hidden, (((0,), (1,)), ((), ())), preferred_element_type=jnp.float32
    )
    term = lax.optimization_barrier(term.astype(jnp.bfloat16))
    summed = lax.psum_scatter(
        term.astype(jnp.float32).astype(jnp.bfloat16), "tp", scatter_dimension=0, tiled=True
    ).astype(jnp.float32)
    back = summed.T.reshape(ep_count, item_rows, share_width)
    returned = lax.all_to_all(
        back.astype(jnp.bfloat16), "ep", split_axis=0, concat_axis=0, tiled=True
    ).astype(back.dtype)
    columns_back = returned.shape[2]
    picked = returned[route_flat, slot_index].reshape(tok_rows, topk, columns_back)
    weighted = jnp.sum(route_weights[:, :, None] * picked, axis=1)
    return weighted.astype(jnp.bfloat16)


def solution(mesh):
    placed = (
        P("ep", None),
        P(),
        P("ep", None),
        P("ep", None),
        P("ep", None, "tp"),
        P("ep", None, "tp"),
        P("ep", "tp", None),
    )
    ep, tp = mesh.shape["ep"], mesh.shape["tp"]

    def whole(tokens, norm_gain, route_ids, route_weights, gate_proj, up_proj, down_proj):
        toks, width = tokens.shape[0] // ep, tokens.shape[1]
        cap = capacity_of(toks, route_ids.shape[1], ep)
        hid = gate_proj.shape[2] // tp
        cube = tp == 2**3 and ep % 2 == 0
        fits = width % (tp * 256) == 0 and hid % 128 == 0 and cap % 16 == 0 and toks % 128 == 0
        body = local_fused if cube and fits else local
        return jax.shard_map(
            body, mesh=mesh, in_specs=placed, out_specs=P("ep", "tp"), check_vma=False
        )(tokens, norm_gain, route_ids, route_weights, gate_proj, up_proj, down_proj)

    return whole
```

```python
import functools

import jax
import jax.numpy as jnp
from jax import lax
from jax.experimental import pallas as pl
from jax.experimental.pallas import tpu as pltpu
from jax.sharding import PartitionSpec as P

MESH = pl.DeviceIdType.MESH
F32, BF16 = jnp.float32, jnp.bfloat16


def dot(a, b):
    return jnp.dot(a, b, preferred_element_type=F32)


def fused(ep, cap, share, chunk, tok, gain, ids, wts, gate_h, up_h, down_h, out, *scratch):
    (normed, pick, rows, outbox, gate_w, up_w, down_w, hidden, to_sib, from_sib, acc, sent, from_diag,
     from_x, from_y, relay, final, back, wsem, ssem, rsem) = scratch
    toks, width = tok.shape
    topk = ids.shape[0]
    hid = hidden.shape[2]
    e = lax.axis_index("ep")
    j = lax.axis_index("tp")
    c, x, y = j % 2, (j // 2) % 2, j // 4

    def at(yy, xx, cc):
        return (yy * 2 + xx) * 2 + cc

    spots = [(y, x), (y, 1 - x), (1 - y, x), (1 - y, 1 - x)]

    def cols(m, core):
        return pl.ds(pl.multiple_of(at(*spots[m], core) * share, share), share)

    x_dev = (e, at(y, 1 - x, c))
    y_dev = (e, at(1 - y, x, c))
    sib = (e, at(y, x, 1 - c))

    loads = [
        pltpu.make_async_copy(h.at[0], v, wsem.at[i])
        for i, (h, v) in enumerate(((gate_h, gate_w), (up_h, up_w), (down_h, down_w)))
    ]
    for load in loads:
        load.start()
    barrier = pltpu.get_barrier_semaphore()
    greeted = [((e + d) % ep, j) for d in range(1, ep)] + [x_dev, y_dev, sib]
    for dev in greeted:
        pl.semaphore_signal(barrier, inc=1, device_id=dev, device_id_type=MESH)

    count = [0]
    started = []

    def remote(src, dst, dev):
        k = count[0]
        count[0] += 1
        copy = pltpu.make_async_remote_copy(
            src_ref=src, dst_ref=dst, send_sem=ssem.at[k], recv_sem=rsem.at[k],
            device_id=dev, device_id_type=MESH,
        )
        started.append(copy)
        copy.start()
        return copy

    near = e + 1 - 2 * (e % 2)
    peers = [e, near, (e + 2) % ep, (near + 2) % ep]

    values = tok[...].astype(F32)
    mean_square = jnp.mean(values * values, axis=-1, keepdims=True)
    normed[...] = (values * lax.rsqrt(mean_square + 1e-06) * gain[...]).astype(BF16)
    turn = lax.broadcasted_iota(jnp.int32, (8, toks), 0)
    experts = jnp.full((8, toks), -1, jnp.int32)
    for i in range(ep):
        experts = jnp.where(turn == i, peers[i], experts)
    named = jnp.zeros(experts.shape, jnp.bool_)
    for k in range(topk):
        named = named | (ids[k : k + 1, :] == experts)
    named = jnp.where(named, 1.0, 0.0)
    before = (
        lax.broadcasted_iota(jnp.int32, (toks, toks), 0)
        < lax.broadcasted_iota(jnp.int32, (toks, toks), 1)
    )
    slot = dot(named.astype(BF16), jnp.where(before, 1.0, 0.0).astype(BF16))
    place = jnp.where(named > 0.5, slot, -1.0)
    slots = lax.broadcasted_iota(jnp.int32, (cap, toks), 0).astype(F32)
    for i in range(ep):
        pick[i] = jnp.where(place[i : i + 1, :] == slots, 1.0, 0.0).astype(BF16)
    mine = cols(0, c)
    for i in range(1, ep):
        outbox[i - 1] = dot(pick[i], normed[:, mine]).astype(BF16)

    pl.semaphore_wait(barrier, len(greeted))
    over_z = {}
    for i in range(1, ep):
        over_z[i] = remote(outbox.at[i - 1], rows.at[i, :, mine], (peers[i], j))
    rows[0] = dot(pick[0], normed[...]).astype(BF16)

    along_x, along_y, diag_1, diag_2 = {}, {}, {}, {}
    over_d2d = {i: [] for i in range(1, ep)}
    quarter = share // 2

    def piece(i, m, part=None):
        if part is None:
            return rows.at[i, :, cols(m, c)]
        start = pl.multiple_of(at(*spots[m], c) * share + part * quarter, quarter)
        return rows.at[i, :, pl.ds(start, quarter)]

    def spread(i):
        over_z[i].wait_recv()
        along_x[i] = remote(piece(i, 0), piece(i, 0), x_dev)
        along_y[i] = remote(piece(i, 0), piece(i, 0), y_dev)
        over_d2d[i].append(remote(piece(i, 0), piece(i, 0), sib))

    def forward(i):
        along_x[i].wait_recv()
        diag_1[i] = remote(piece(i, 1, 0), piece(i, 1, 0), y_dev)
        along_y[i].wait_recv()
        diag_2[i] = remote(piece(i, 2, 1), piece(i, 2, 1), x_dev)
        over_d2d[i].append(remote(piece(i, 1), piece(i, 1), sib))
        over_d2d[i].append(remote(piece(i, 2), piece(i, 2), sib))

    def across(i):
        diag_1[i].wait_recv()
        diag_2[i].wait_recv()
        over_d2d[i].append(remote(piece(i, 3), piece(i, 3), sib))

    def gathered(i):
        for copy in over_d2d[i]:
            copy.wait_recv()

    pace = hid // chunk

    def gate_up(g, n):
        at_n = pl.ds(n * chunk, chunk)
        held = rows[2 * g : 2 * g + 2].reshape(2 * cap, width)
        gate_act = dot(held, gate_w[:, at_n])
        up_act = dot(held, up_w[:, at_n])
        hidden[g, :, at_n] = (gate_act / (1.0 + jnp.exp(-gate_act)) * up_act).astype(BF16)

    def gate_up_with(g, steps):
        for n in range(pace):
            gate_up(g, n)
            first = n * len(steps) // pace
            for step in steps[first : (n + 1) * len(steps) // pace]:
                step()

    pair, sends = {}, {}
    low, high = pl.ds(0, cap), pl.ds(cap, cap)

    def compute(g, m):
        to_sib[g, m] = dot(hidden[g], down_w[:, cols(m, 1 - c)]).astype(BF16)
        pair[g, m] = remote(to_sib.at[g, m], from_sib.at[g, m], sib)
        acc[g, m] = dot(hidden[g], down_w[:, cols(m, c)])

    def join(g, m):
        pair[g, m].wait_recv()
        along = acc[g, m] + from_sib[g, m].astype(F32)
        if m == 3:
            sent[g, 0] = along.astype(BF16)
            sends[g, "diag_a"] = remote(sent.at[g, 0, low], from_diag.at[g, 0], x_dev)
            sends[g, "diag_b"] = remote(sent.at[g, 0, high], from_diag.at[g, 1], y_dev)
            return
        acc[g, m] = along
        if m == 1:
            sent[g, 1, :cap] = along[:cap].astype(BF16)
            sends[g, "x_a"] = remote(sent.at[g, 1, low], from_x.at[g, 0], x_dev)
        if m == 2:
            sent[g, 2, cap:] = along[cap:].astype(BF16)
            sends[g, "y_b"] = remote(sent.at[g, 2, high], from_y.at[g, 1], y_dev)

    def pass_on(g):
        sends[g, "diag_a"].wait_recv()
        relay[g, 0] = (acc[g, 2, :cap] + from_diag[g, 0].astype(F32)).astype(BF16)
        sends[g, "y_a"] = remote(relay.at[g, 0], from_y.at[g, 0], y_dev)
        sends[g, "diag_b"].wait_recv()
        relay[g, 1] = (acc[g, 1, cap:] + from_diag[g, 1].astype(F32)).astype(BF16)
        sends[g, "x_b"] = remote(relay.at[g, 1], from_x.at[g, 1], x_dev)

    def down(g):
        compute(g, 3)
        compute(g, 1)
        join(g, 3)
        compute(g, 2)
        join(g, 1)
        compute(g, 0)
        join(g, 2)

    homeward = {}

    def finish(g):
        for i, (one, two) in enumerate((("x_a", "y_a"), ("y_b", "x_b"))):
            sends[g, one].wait_recv()
            sends[g, two].wait_recv()
            part = acc[g, 0, i * cap : (i + 1) * cap]
            part = part + from_x[g, i].astype(F32) + from_y[g, i].astype(F32)
            p = 2 * g + i
            final[p] = part.astype(BF16)
            if p:
                homeward[p] = remote(final.at[p], back.at[p], (peers[p], j))

    spread(1)
    forward(1)
    spread(2)
    across(1)
    spread(3)
    loads[0].wait()
    loads[1].wait()
    gathered(1)
    gate_up_with(0, [
        lambda: forward(2), lambda: forward(3), lambda: across(2), lambda: across(3),
    ])
    loads[2].wait()
    down(0)
    gathered(2)
    gathered(3)
    gate_up_with(1, [lambda: pass_on(0), lambda: join(0, 0), lambda: finish(0)])
    down(1)
    pass_on(1)
    join(1, 0)
    finish(1)

    eye = (
        lax.broadcasted_iota(jnp.int32, (toks, toks), 0)
        == lax.broadcasted_iota(jnp.int32, (toks, toks), 1)
    )

    def weighted(i, value):
        scale = jnp.zeros((1, toks), F32)
        for k in range(topk):
            scale = scale + jnp.where(ids[k : k + 1, :] == peers[i], wts[k : k + 1, :], 0.0)
        scale = jnp.sum(jnp.where(eye, scale, 0.0), axis=1, keepdims=True)
        got = lax.dot_general(
            pick[i], value, (((0,), (0,)), ((), ())), preferred_element_type=F32
        )
        return scale * got

    mixed = weighted(0, final[0])
    for i in range(1, ep):
        homeward[i].wait_recv()
        mixed = mixed + weighted(i, back[i])
    out[...] = mixed.astype(out.dtype)
    for copy in started:
        copy.wait_send()


def local_fused(tokens, norm_gain, route_ids, route_weights, gate_proj, up_proj, down_proj):
    ep = lax.axis_size("ep")
    tp = lax.axis_size("tp")
    toks, width = tokens.shape
    topk = route_ids.shape[1]
    hid = gate_proj.shape[2]
    cap = capacity_of(toks, topk, ep)
    share = width // tp
    total = ep * cap
    chunk = next(n for n in (256, 128) if hid % n == 0)
    others = ep - 1
    copies = 9 * others + 2 * (4 + 6) + others
    vmem = pl.BlockSpec(memory_space=pltpu.VMEM)
    hbm = pl.BlockSpec(memory_space=pltpu.HBM)
    flops = 6 * total * width * hid
    return pl.pallas_call(
        functools.partial(fused, ep, cap, share, chunk),
        out_shape=jax.ShapeDtypeStruct((toks, share), BF16),
        in_specs=[vmem] * 4 + [hbm] * 3,
        out_specs=vmem,
        scratch_shapes=[
            pltpu.VMEM((toks, width), BF16),
            pltpu.VMEM((ep, cap, toks), BF16),
            pltpu.VMEM((ep, cap, width), BF16),
            pltpu.VMEM((others, cap, share), BF16),
            pltpu.VMEM((width, hid), BF16),
            pltpu.VMEM((width, hid), BF16),
            pltpu.VMEM((hid, width), BF16),
            pltpu.VMEM((2, 2 * cap, hid), BF16),
            pltpu.VMEM((2, 4, 2 * cap, share), BF16),
            pltpu.VMEM((2, 4, 2 * cap, share), BF16),
            pltpu.VMEM((2, 4, 2 * cap, share), F32),
            pltpu.VMEM((2, 3, 2 * cap, share), BF16),
            pltpu.VMEM((2, 2, cap, share), BF16),
            pltpu.VMEM((2, 2, cap, share), BF16),
            pltpu.VMEM((2, 2, cap, share), BF16),
            pltpu.VMEM((2, 2, cap, share), BF16),
            pltpu.VMEM((ep, cap, share), BF16),
            pltpu.VMEM((ep, cap, share), BF16),
            pltpu.SemaphoreType.DMA((3,)),
            pltpu.SemaphoreType.DMA((copies,)),
            pltpu.SemaphoreType.DMA((copies,)),
        ],
        compiler_params=pltpu.CompilerParams(
            collective_id=0, has_side_effects=True, vmem_limit_bytes=56 * 1024 * 1024
        ),
        cost_estimate=pl.CostEstimate(
            flops=flops, bytes_accessed=6 * width * hid, transcendentals=total * hid
        ),
    )(
        tokens, norm_gain.reshape(1, width), route_ids.T, route_weights.T,
        gate_proj, up_proj, down_proj,
    )


def capacity_of(tok_rows, topk, ep_count):
    return min(tok_rows, (3 * tok_rows * topk + 2 * ep_count - 1) // (2 * ep_count))


def local(tokens, norm_gain, route_ids, route_weights, gate_proj, up_proj, down_proj):
    ep_count = lax.axis_size("ep")
    tp_count = lax.axis_size("tp")
    tok_rows, width = tokens.shape
    topk = route_ids.shape[1]
    capacity = min(tok_rows, (3 * tok_rows * topk + 2 * ep_count - 1) // (2 * ep_count))
    share_width = width // tp_count
    values = tokens.astype(jnp.float32)
    mean_square = jnp.mean(values * values, axis=-1, keepdims=True)
    normed = (values * lax.rsqrt(mean_square + 1e-06) * norm_gain).astype(jnp.bfloat16)
    route_flat = route_ids.reshape(-1)
    onehot = (route_flat[:, None] == jnp.arange(ep_count, dtype=jnp.int32)[None, :]).astype(
        jnp.int32
    )
    slot_index = jnp.sum((jnp.cumsum(onehot, axis=0) - onehot) * onehot, axis=1)
    repeated = jnp.repeat(normed, topk, axis=0)
    down_local = down_proj[0]
    outgoing = (
        jnp.zeros((ep_count, capacity, width), jnp.bfloat16)
        .at[route_flat, slot_index]
        .set(repeated)
    )
    arrived = lax.all_to_all(outgoing, "ep", split_axis=0, concat_axis=0, tiled=True)
    item_rows = arrived.shape[1]
    merged_rows = arrived.reshape(-1, width)
    gate_act = jnp.dot(merged_rows, gate_proj[0], preferred_element_type=jnp.float32)
    up_act = jnp.dot(merged_rows, up_proj[0], preferred_element_type=jnp.float32)
    hidden = (jax.nn.silu(gate_act) * up_act).astype(jnp.bfloat16)
    term = lax.dot_general(
        down_local, hidden, (((0,), (1,)), ((), ())), preferred_element_type=jnp.float32
    )
    term = lax.optimization_barrier(term.astype(jnp.bfloat16))
    summed = lax.psum_scatter(
        term.astype(jnp.float32).astype(jnp.bfloat16), "tp", scatter_dimension=0, tiled=True
    ).astype(jnp.float32)
    back = summed.T.reshape(ep_count, item_rows, share_width)
    returned = lax.all_to_all(
        back.astype(jnp.bfloat16), "ep", split_axis=0, concat_axis=0, tiled=True
    ).astype(back.dtype)
    columns_back = returned.shape[2]
    picked = returned[route_flat, slot_index].reshape(tok_rows, topk, columns_back)
    weighted = jnp.sum(route_weights[:, :, None] * picked, axis=1)
    return weighted.astype(jnp.bfloat16)


def solution(mesh):
    placed = (
        P("ep", None),
        P(),
        P("ep", None),
        P("ep", None),
        P("ep", None, "tp"),
        P("ep", None, "tp"),
        P("ep", "tp", None),
    )
    ep, tp = mesh.shape["ep"], mesh.shape["tp"]

    def whole(tokens, norm_gain, route_ids, route_weights, gate_proj, up_proj, down_proj):
        toks, width = tokens.shape[0] // ep, tokens.shape[1]
        cap = capacity_of(toks, route_ids.shape[1], ep)
        hid = gate_proj.shape[2] // tp
        cube = tp == 2**3 and ep == 2**2
        fits = width % (tp * 256) == 0 and hid % 128 == 0 and cap % 16 == 0 and toks % 128 == 0
        body = local_fused if cube and fits else local
        return jax.shard_map(
            body, mesh=mesh, in_specs=placed, out_specs=P("ep", "tp"), check_vma=False
        )(tokens, norm_gain, route_ids, route_weights, gate_proj, up_proj, down_proj)

    return whole
```

```python
import functools

import jax
import jax.numpy as jnp
from jax import lax
from jax.experimental import pallas as pl
from jax.experimental.pallas import tpu as pltpu
from jax.sharding import PartitionSpec as P

MESH = pl.DeviceIdType.MESH
F32, BF16 = jnp.float32, jnp.bfloat16


def dot(a, b):
    return jnp.dot(a, b, preferred_element_type=F32)


def fused(ep, cap, share, chunk, tok, gain, ids, wts, gate_h, up_h, down_h, out, *scratch):
    (normed, pick, rows, outbox, gate_w, up_w, down_w, hidden, to_sib, from_sib, acc, sent, from_diag,
     from_x, from_y, relay, final, back, wsem, ssem, rsem) = scratch
    toks, width = tok.shape
    topk = ids.shape[0]
    hid = hidden.shape[2]
    e = lax.axis_index("ep")
    j = lax.axis_index("tp")
    c, x, y = j % 2, (j // 2) % 2, j // 4

    def at(yy, xx, cc):
        return (yy * 2 + xx) * 2 + cc

    spots = [(y, x), (y, 1 - x), (1 - y, x), (1 - y, 1 - x)]

    def cols(m, core):
        return pl.ds(pl.multiple_of(at(*spots[m], core) * share, share), share)

    x_dev = (e, at(y, 1 - x, c))
    y_dev = (e, at(1 - y, x, c))
    sib = (e, at(y, x, 1 - c))

    loads = [
        pltpu.make_async_copy(h.at[0], v, wsem.at[i])
        for i, (h, v) in enumerate(((gate_h, gate_w), (up_h, up_w), (down_h, down_w)))
    ]
    for load in loads:
        load.start()
    barrier = pltpu.get_barrier_semaphore()
    greeted = [((e + d) % ep, j) for d in range(1, ep)] + [x_dev, y_dev, sib]
    for dev in greeted:
        pl.semaphore_signal(barrier, inc=1, device_id=dev, device_id_type=MESH)

    count = [0]
    started = []

    def remote(src, dst, dev):
        k = count[0]
        count[0] += 1
        copy = pltpu.make_async_remote_copy(
            src_ref=src, dst_ref=dst, send_sem=ssem.at[k], recv_sem=rsem.at[k],
            device_id=dev, device_id_type=MESH,
        )
        started.append(copy)
        copy.start()
        return copy

    near = e + 1 - 2 * (e % 2)
    peers = [e, near, (e + 2) % ep, (near + 2) % ep]

    values = tok[...].astype(F32)
    mean_square = jnp.mean(values * values, axis=-1, keepdims=True)
    normed[...] = (values * lax.rsqrt(mean_square + 1e-06) * gain[...]).astype(BF16)
    turn = lax.broadcasted_iota(jnp.int32, (8, toks), 0)
    experts = jnp.full((8, toks), -1, jnp.int32)
    for i in range(ep):
        experts = jnp.where(turn == i, peers[i], experts)
    named = jnp.zeros(experts.shape, jnp.bool_)
    for k in range(topk):
        named = named | (ids[k : k + 1, :] == experts)
    named = jnp.where(named, 1.0, 0.0)
    before = (
        lax.broadcasted_iota(jnp.int32, (toks, toks), 0)
        < lax.broadcasted_iota(jnp.int32, (toks, toks), 1)
    )
    slot = dot(named.astype(BF16), jnp.where(before, 1.0, 0.0).astype(BF16))
    place = jnp.where(named > 0.5, slot, -1.0)
    slots = lax.broadcasted_iota(jnp.int32, (cap, toks), 0).astype(F32)
    for i in range(ep):
        pick[i] = jnp.where(place[i : i + 1, :] == slots, 1.0, 0.0).astype(BF16)
    mine = cols(0, c)
    for i in range(1, ep):
        outbox[i - 1] = dot(pick[i], normed[:, mine]).astype(BF16)

    pl.semaphore_wait(barrier, len(greeted))
    over_z = {}
    for i in range(1, ep):
        over_z[i] = remote(outbox.at[i - 1], rows.at[i, :, mine], (peers[i], j))
    rows[0] = dot(pick[0], normed[...]).astype(BF16)

    along_x, along_y, diag_1, diag_2 = {}, {}, {}, {}
    over_d2d = {i: [] for i in range(1, ep)}
    quarter = share // 2

    def piece(i, m, part=None):
        if part is None:
            return rows.at[i, :, cols(m, c)]
        start = pl.multiple_of(at(*spots[m], c) * share + part * quarter, quarter)
        return rows.at[i, :, pl.ds(start, quarter)]

    def spread(i):
        over_z[i].wait_recv()
        along_x[i] = remote(piece(i, 0), piece(i, 0), x_dev)
        along_y[i] = remote(piece(i, 0), piece(i, 0), y_dev)
        over_d2d[i].append(remote(piece(i, 0), piece(i, 0), sib))

    def forward(i):
        along_x[i].wait_recv()
        diag_1[i] = remote(piece(i, 1, 0), piece(i, 1, 0), y_dev)
        along_y[i].wait_recv()
        diag_2[i] = remote(piece(i, 2, 1), piece(i, 2, 1), x_dev)
        over_d2d[i].append(remote(piece(i, 1), piece(i, 1), sib))
        over_d2d[i].append(remote(piece(i, 2), piece(i, 2), sib))

    def across(i):
        diag_1[i].wait_recv()
        diag_2[i].wait_recv()
        over_d2d[i].append(remote(piece(i, 3), piece(i, 3), sib))

    def gathered(i):
        for copy in over_d2d[i]:
            copy.wait_recv()

    pace = hid // chunk

    def gate_up(g, n):
        at_n = pl.ds(n * chunk, chunk)
        held = rows[2 * g : 2 * g + 2].reshape(2 * cap, width)
        gate_act = dot(held, gate_w[:, at_n])
        up_act = dot(held, up_w[:, at_n])
        hidden[g, :, at_n] = (gate_act / (1.0 + jnp.exp(-gate_act)) * up_act).astype(BF16)

    def gate_up_with(g, steps):
        for n in range(pace):
            gate_up(g, n)
            first = n * len(steps) // pace
            for step in steps[first : (n + 1) * len(steps) // pace]:
                step()

    pair, sends = {}, {}
    low, high = pl.ds(0, cap), pl.ds(cap, cap)

    def compute(g, m):
        to_sib[g, m] = dot(hidden[g], down_w[:, cols(m, 1 - c)]).astype(BF16)
        pair[g, m] = remote(to_sib.at[g, m], from_sib.at[g, m], sib)
        acc[g, m] = dot(hidden[g], down_w[:, cols(m, c)])

    def join(g, m):
        pair[g, m].wait_recv()
        along = acc[g, m] + from_sib[g, m].astype(F32)
        if m == 3:
            sent[g, 0] = along.astype(BF16)
            sends[g, "diag_a"] = remote(sent.at[g, 0, low], from_diag.at[g, 0], x_dev)
            sends[g, "diag_b"] = remote(sent.at[g, 0, high], from_diag.at[g, 1], y_dev)
            return
        acc[g, m] = along
        if m == 1:
            sent[g, 1, :cap] = along[:cap].astype(BF16)
            sends[g, "x_a"] = remote(sent.at[g, 1, low], from_x.at[g, 0], x_dev)
        if m == 2:
            sent[g, 2, cap:] = along[cap:].astype(BF16)
            sends[g, "y_b"] = remote(sent.at[g, 2, high], from_y.at[g, 1], y_dev)

    def pass_on(g):
        sends[g, "diag_a"].wait_recv()
        relay[g, 0] = (acc[g, 2, :cap] + from_diag[g, 0].astype(F32)).astype(BF16)
        sends[g, "y_a"] = remote(relay.at[g, 0], from_y.at[g, 0], y_dev)
        sends[g, "diag_b"].wait_recv()
        relay[g, 1] = (acc[g, 1, cap:] + from_diag[g, 1].astype(F32)).astype(BF16)
        sends[g, "x_b"] = remote(relay.at[g, 1], from_x.at[g, 1], x_dev)

    def down(g):
        compute(g, 3)
        compute(g, 1)
        join(g, 3)
        compute(g, 2)
        join(g, 1)
        compute(g, 0)
        join(g, 2)

    homeward = {}

    def finish(g):
        for i, (one, two) in enumerate((("x_a", "y_a"), ("y_b", "x_b"))):
            sends[g, one].wait_recv()
            sends[g, two].wait_recv()
            part = acc[g, 0, i * cap : (i + 1) * cap]
            part = part + from_x[g, i].astype(F32) + from_y[g, i].astype(F32)
            p = 2 * g + i
            final[p] = part.astype(BF16)
            if p:
                homeward[p] = remote(final.at[p], back.at[p], (peers[p], j))

    spread(1)
    forward(1)
    spread(2)
    across(1)
    loads[0].wait()
    loads[1].wait()
    gathered(1)
    gate_up_with(0, [
        lambda: spread(3), lambda: forward(2), lambda: forward(3), lambda: across(2), lambda: across(3),
    ])
    loads[2].wait()
    down(0)
    gathered(2)
    gathered(3)
    gate_up_with(1, [lambda: pass_on(0), lambda: join(0, 0), lambda: finish(0)])
    down(1)
    pass_on(1)
    join(1, 0)
    finish(1)

    eye = (
        lax.broadcasted_iota(jnp.int32, (toks, toks), 0)
        == lax.broadcasted_iota(jnp.int32, (toks, toks), 1)
    )

    def weighted(i, value):
        scale = jnp.zeros((1, toks), F32)
        for k in range(topk):
            scale = scale + jnp.where(ids[k : k + 1, :] == peers[i], wts[k : k + 1, :], 0.0)
        scale = jnp.sum(jnp.where(eye, scale, 0.0), axis=1, keepdims=True)
        got = lax.dot_general(
            pick[i], value, (((0,), (0,)), ((), ())), preferred_element_type=F32
        )
        return scale * got

    mixed = weighted(0, final[0])
    for i in range(1, ep):
        homeward[i].wait_recv()
        mixed = mixed + weighted(i, back[i])
    out[...] = mixed.astype(out.dtype)
    for copy in started:
        copy.wait_send()


def local_fused(tokens, norm_gain, route_ids, route_weights, gate_proj, up_proj, down_proj):
    ep = lax.axis_size("ep")
    tp = lax.axis_size("tp")
    toks, width = tokens.shape
    topk = route_ids.shape[1]
    hid = gate_proj.shape[2]
    cap = capacity_of(toks, topk, ep)
    share = width // tp
    total = ep * cap
    chunk = next(n for n in (256, 128) if hid % n == 0)
    others = ep - 1
    copies = 9 * others + 2 * (4 + 6) + others
    vmem = pl.BlockSpec(memory_space=pltpu.VMEM)
    hbm = pl.BlockSpec(memory_space=pltpu.HBM)
    flops = 6 * total * width * hid
    return pl.pallas_call(
        functools.partial(fused, ep, cap, share, chunk),
        out_shape=jax.ShapeDtypeStruct((toks, share), BF16),
        in_specs=[vmem] * 4 + [hbm] * 3,
        out_specs=vmem,
        scratch_shapes=[
            pltpu.VMEM((toks, width), BF16),
            pltpu.VMEM((ep, cap, toks), BF16),
            pltpu.VMEM((ep, cap, width), BF16),
            pltpu.VMEM((others, cap, share), BF16),
            pltpu.VMEM((width, hid), BF16),
            pltpu.VMEM((width, hid), BF16),
            pltpu.VMEM((hid, width), BF16),
            pltpu.VMEM((2, 2 * cap, hid), BF16),
            pltpu.VMEM((2, 4, 2 * cap, share), BF16),
            pltpu.VMEM((2, 4, 2 * cap, share), BF16),
            pltpu.VMEM((2, 4, 2 * cap, share), F32),
            pltpu.VMEM((2, 3, 2 * cap, share), BF16),
            pltpu.VMEM((2, 2, cap, share), BF16),
            pltpu.VMEM((2, 2, cap, share), BF16),
            pltpu.VMEM((2, 2, cap, share), BF16),
            pltpu.VMEM((2, 2, cap, share), BF16),
            pltpu.VMEM((ep, cap, share), BF16),
            pltpu.VMEM((ep, cap, share), BF16),
            pltpu.SemaphoreType.DMA((3,)),
            pltpu.SemaphoreType.DMA((copies,)),
            pltpu.SemaphoreType.DMA((copies,)),
        ],
        compiler_params=pltpu.CompilerParams(
            collective_id=0, has_side_effects=True, vmem_limit_bytes=56 * 1024 * 1024
        ),
        cost_estimate=pl.CostEstimate(
            flops=flops, bytes_accessed=6 * width * hid, transcendentals=total * hid
        ),
    )(
        tokens, norm_gain.reshape(1, width), route_ids.T, route_weights.T,
        gate_proj, up_proj, down_proj,
    )


def capacity_of(tok_rows, topk, ep_count):
    return min(tok_rows, (3 * tok_rows * topk + 2 * ep_count - 1) // (2 * ep_count))


def local(tokens, norm_gain, route_ids, route_weights, gate_proj, up_proj, down_proj):
    ep_count = lax.axis_size("ep")
    tp_count = lax.axis_size("tp")
    tok_rows, width = tokens.shape
    topk = route_ids.shape[1]
    capacity = min(tok_rows, (3 * tok_rows * topk + 2 * ep_count - 1) // (2 * ep_count))
    share_width = width // tp_count
    values = tokens.astype(jnp.float32)
    mean_square = jnp.mean(values * values, axis=-1, keepdims=True)
    normed = (values * lax.rsqrt(mean_square + 1e-06) * norm_gain).astype(jnp.bfloat16)
    route_flat = route_ids.reshape(-1)
    onehot = (route_flat[:, None] == jnp.arange(ep_count, dtype=jnp.int32)[None, :]).astype(
        jnp.int32
    )
    slot_index = jnp.sum((jnp.cumsum(onehot, axis=0) - onehot) * onehot, axis=1)
    repeated = jnp.repeat(normed, topk, axis=0)
    down_local = down_proj[0]
    outgoing = (
        jnp.zeros((ep_count, capacity, width), jnp.bfloat16)
        .at[route_flat, slot_index]
        .set(repeated)
    )
    arrived = lax.all_to_all(outgoing, "ep", split_axis=0, concat_axis=0, tiled=True)
    item_rows = arrived.shape[1]
    merged_rows = arrived.reshape(-1, width)
    gate_act = jnp.dot(merged_rows, gate_proj[0], preferred_element_type=jnp.float32)
    up_act = jnp.dot(merged_rows, up_proj[0], preferred_element_type=jnp.float32)
    hidden = (jax.nn.silu(gate_act) * up_act).astype(jnp.bfloat16)
    term = lax.dot_general(
        down_local, hidden, (((0,), (1,)), ((), ())), preferred_element_type=jnp.float32
    )
    term = lax.optimization_barrier(term.astype(jnp.bfloat16))
    summed = lax.psum_scatter(
        term.astype(jnp.float32).astype(jnp.bfloat16), "tp", scatter_dimension=0, tiled=True
    ).astype(jnp.float32)
    back = summed.T.reshape(ep_count, item_rows, share_width)
    returned = lax.all_to_all(
        back.astype(jnp.bfloat16), "ep", split_axis=0, concat_axis=0, tiled=True
    ).astype(back.dtype)
    columns_back = returned.shape[2]
    picked = returned[route_flat, slot_index].reshape(tok_rows, topk, columns_back)
    weighted = jnp.sum(route_weights[:, :, None] * picked, axis=1)
    return weighted.astype(jnp.bfloat16)


def solution(mesh):
    placed = (
        P("ep", None),
        P(),
        P("ep", None),
        P("ep", None),
        P("ep", None, "tp"),
        P("ep", None, "tp"),
        P("ep", "tp", None),
    )
    ep, tp = mesh.shape["ep"], mesh.shape["tp"]

    def whole(tokens, norm_gain, route_ids, route_weights, gate_proj, up_proj, down_proj):
        toks, width = tokens.shape[0] // ep, tokens.shape[1]
        cap = capacity_of(toks, route_ids.shape[1], ep)
        hid = gate_proj.shape[2] // tp
        cube = tp == 2**3 and ep == 2**2
        fits = width % (tp * 256) == 0 and hid % 128 == 0 and cap % 16 == 0 and toks % 128 == 0
        body = local_fused if cube and fits else local
        return jax.shard_map(
            body, mesh=mesh, in_specs=placed, out_specs=P("ep", "tp"), check_vma=False
        )(tokens, norm_gain, route_ids, route_weights, gate_proj, up_proj, down_proj)

    return whole
```
